32 devices in a mesh: rep: 2 (over x), fs: 8 (over z, y), tp: 2 (over core).
Axes of the slice: x: 2, y: 2, z: 4, core: 2. Of those that a mesh axis runs over, the one named last changes fastest.
Arguments:
- tokens: bfloat16 [16, 384, 2048], P(('rep', 'fs')), may hold values from -6 to 6
- mix_gain: float32 [2048], replicated, may hold values from 0.1 to 1.9
- value_weight: float32 [2048, 2048], P('fs', 'tp'), may hold values from -0.125 to 0.125
- value_scale: float32 [2048], P(('tp', 'fs')), may hold values from 0.5 to 2
- inner_weight: float32 [2048, 2048], P('fs', 'tp'), may hold values from -0.125 to 0.125
- inner_scale: float32 [2048], P(('tp', 'fs')), may hold values from 0.5 to 2
- outer_weight: float32 [2048, 2048], P('fs', 'tp'), may hold values from -0.125 to 0.125
- outer_scale: float32 [2048], P(('tp', 'fs')), may hold values from 0.5 to 2
- conv_taps: float32 [3, 2048], P(None, 'tp'), may hold values from -3 to 3
- out_weight: float32 [2048, 2048], P('tp', 'fs'), may hold values from -0.125 to 0.125
- out_scale: float32 [2048], P('fs'), may hold values from 0.5 to 2
- mlp_gain: float32 [2048], replicated, may hold values from 0.1 to 1.9
- up_weight: float32 [2048, 6144], P('fs', 'tp'), may hold values from -0.125 to 0.125
- up_scale: float32 [6144], P(('tp', 'fs')), may hold values from 0.5 to 2
- down_weight: float32 [6144, 2048], P('tp', 'fs'), may hold values from -0.078125 to 0.078125
- down_scale: float32 [2048], P('fs'), may hold values from 0.5 to 2
Outputs:
- layer_out: bfloat16 [16, 384, 2048], P(('rep', 'fs'))
The draws below stay inside these ranges and needn't reach their ends.
All inputs are finite; a program needn't handle non-finite values.
Results may differ from the reference program's by a relative error of at most 0.02.
Values may be sent and summed in bfloat16 or wider, within the bound.
A program may use at most 128 MiB of HBM per device.

```python
import math
import jax
import jax.numpy as jnp
from jax import lax

D = 2048
FF = 6144
TOK_DEV = 384
SEQS = 16
N_TP = 2


def block_scale(rng, dims, shards, low, high):
    def one(axis_at, shards_of):
        heights = jax.random.uniform(jax.random.fold_in(jax.random.fold_in(rng, 6), axis_at), (shards_of,), jnp.float32, low / len(shards), high / len(shards))
        return jnp.repeat(jnp.exp(heights), dims[axis_at] // shards_of).reshape((-1,) + (1,) * (len(dims) - axis_at - 1))

    level = one(*shards[0])
    for cut in shards[1:]:
        level = level * one(*cut)
    return level


def scatter_about(key, shape, scale, limit, cuts=(), kind=jnp.bfloat16):
    values = scale * jax.random.normal(key, shape, jnp.float32)
    if cuts:
        values = values * block_scale(key, shape, cuts, -0.22, 0.18)
    return jnp.clip(values, -limit, limit).astype(kind)


def setup_inputs(seed: int = 0) -> dict:
    key_of = jax.random.split(jax.random.key(seed), 17)
    return {
        "tokens": scatter_about(key_of[0], (SEQS, TOK_DEV, D), 1.0, 6.0, ((0, 16),)),
        "mix_gain": jnp.clip(1.0 + 0.18 * jax.random.normal(key_of[1], (D,), jnp.float32), 0.1, 1.9),
        "value_weight": scatter_about(key_of[2], (D, D), D ** -0.5, 0.125, ((0, 8), (1, 2)), jnp.float32),
        "value_scale": jnp.clip(jnp.exp(math.log(2.0) - 1.3862944 * jax.random.uniform(key_of[3], (D,), jnp.float32) ** block_scale(key_of[3], (D,), ((0, 16),), -0.2, 0.2)), 0.5, 2.0),
        "inner_weight": scatter_about(key_of[4], (D, D), D ** -0.5, 0.125, ((0, 8), (1, 2)), jnp.float32),
        "inner_scale": jnp.clip(jnp.exp(math.log(2.0) - 1.3862944 * jax.random.uniform(key_of[5], (D,), jnp.float32) ** block_scale(key_of[5], (D,), ((0, 16),), -0.2, 0.2)), 0.5, 2.0),
        "outer_weight": scatter_about(key_of[6], (D, D), D ** -0.5, 0.125, ((0, 8), (1, 2)), jnp.float32),
        "outer_scale": jnp.clip(jnp.exp(math.log(2.0) - 1.3862944 * jax.random.uniform(key_of[7], (D,), jnp.float32) ** block_scale(key_of[7], (D,), ((0, 16),), -0.2, 0.2)), 0.5, 2.0),
        "conv_taps": scatter_about(key_of[8], (3, D), 0.6, 3.0, ((1, 2),), jnp.float32),
        "out_weight": scatter_about(key_of[9], (D, D), D ** -0.5, 0.125, ((0, 2), (1, 8)), jnp.float32),
        "out_scale": jnp.clip(jnp.exp(math.log(2.0) - 1.3862944 * jax.random.uniform(key_of[10], (D,), jnp.float32) ** block_scale(key_of[10], (D,), ((0, 8),), -0.2, 0.2)), 0.5, 2.0),
        "mlp_gain": jnp.clip(1.0 + 0.18 * jax.random.normal(key_of[11], (D,), jnp.float32), 0.1, 1.9),
        "up_weight": scatter_about(key_of[12], (D, FF), D ** -0.5, 0.125, ((0, 8), (1, 2)), jnp.float32),
        "up_scale": jnp.clip(jnp.exp(math.log(2.0) - 1.3862944 * jax.random.uniform(key_of[13], (FF,), jnp.float32) ** block_scale(key_of[13], (FF,), ((0, 16),), -0.2, 0.2)), 0.5, 2.0),
        "down_weight": scatter_about(key_of[14], (FF, D), FF ** -0.5, 0.078125, ((0, 2), (1, 8)), jnp.float32),
        "down_scale": jnp.clip(jnp.exp(math.log(2.0) - 1.3862944 * jax.random.uniform(key_of[15], (D,), jnp.float32) ** block_scale(key_of[15], (D,), ((0, 8),), -0.2, 0.2)), 0.5, 2.0),
    }


norm_eps = 1e-06

def normalize(values, gain):
    return values * lax.rsqrt(lax.optimization_barrier(jnp.mean(values * values, axis=-1, keepdims=True)) + norm_eps) * gain

def block_sum(left, right, blocks):
    rows = left.shape[0]
    width = left.shape[1] // blocks
    left_blocks = left.reshape(rows, blocks, width).astype(jnp.float32)
    right_blocks = right.reshape(blocks, width, right.shape[1]).astype(jnp.float32)
    parts = jnp.einsum('lnk,nkd->nld', left_blocks, right_blocks).astype(jnp.bfloat16)
    parts = lax.optimization_barrier(parts)
    return lax.optimization_barrier(jnp.sum(parts.astype(jnp.float32), axis=0))

def reference(tokens, mix_gain, value_weight, value_scale, inner_weight, inner_scale, outer_weight, outer_scale, conv_taps, out_weight, out_scale, mlp_gain, up_weight, up_scale, down_weight, down_scale):
    value_b = value_weight.astype(jnp.bfloat16)
    inner_b = inner_weight.astype(jnp.bfloat16)
    outer_b = outer_weight.astype(jnp.bfloat16)
    out_b = out_weight.astype(jnp.bfloat16)
    up_b = up_weight.astype(jnp.bfloat16)
    down_b = down_weight.astype(jnp.bfloat16)

    def one_sequence(sequence):
        start = sequence.astype(jnp.float32)
        normed = normalize(start, mix_gain).astype(jnp.bfloat16)
        value = jnp.dot(normed, value_b, preferred_element_type=jnp.float32) * value_scale
        inner = jnp.dot(normed, inner_b, preferred_element_type=jnp.float32) * inner_scale
        outer = jnp.dot(normed, outer_b, preferred_element_type=jnp.float32) * outer_scale
        gated = inner * value
        padded = jnp.pad(gated, ((1, 1), (0, 0)))
        conv = conv_taps[0] * padded[:-2] + conv_taps[1] * padded[1:-1] + conv_taps[2] * padded[2:]
        hidden = (outer * conv).astype(jnp.bfloat16)
        middle = start + block_sum(hidden, out_b, N_TP) * out_scale
        normed_mid = normalize(middle, mlp_gain).astype(jnp.bfloat16)
        upper = jnp.dot(normed_mid, up_b, preferred_element_type=jnp.float32) * up_scale
        act = jnp.square(jax.nn.relu(upper)).astype(jnp.bfloat16)
        return (middle + block_sum(act, down_b, N_TP) * down_scale).astype(jnp.bfloat16)
    return lax.map(one_sequence, tokens)
```

```python
import functools

import jax
import jax.numpy as jnp
from jax import lax
from jax.experimental import pallas as pl
from jax.experimental.pallas import tpu as pltpu
from jax.sharding import PartitionSpec as P

MESH = pl.DeviceIdType.MESH
norm_eps = 1e-06
HALO = 16
TILE = 16
f32 = jnp.float32
bf16 = jnp.bfloat16


def kernel(
    nz, G, T, win, rows,
    tok, g1, g2, asc, taps, usc, oc, dc, wa, wo, wu, wd,
    out,
    WA, WO, WU, WD, nrm, hid, p1, q1, mid32, mid, act, p2, q2,
    rz, rd, sz, sd, sy, loc, rn, sn, r1, s1, ra, sa, r2, s2, ro, so,
):
    D = tok.shape[1]
    pw = D // nz
    cw = pw // 2
    r, f, t = lax.axis_index("rep"), lax.axis_index("fs"), lax.axis_index("tp")
    z, y = f // 2, f % 2
    fy = z * 2 + 1 - y
    g = r * 2 + y
    srcs = (wa, wo, wu, wd)
    ka, ko, ku, kd = (w.shape[1] for w in srcs)
    has_lo, has_hi = z > 0, z < nz - 1
    if T == 2:
        start, off = t * (rows - HALO), t * HALO
    else:
        start = jnp.clip(t * rows - HALO, 0, tok.shape[0] - win)
        off = t * rows - start
    start, off = pl.multiple_of(start, HALO), pl.multiple_of(off, HALO)

    def member(m):
        return (m // 2, z * 2 + m % 2, t)

    def others():
        return [(g + d) % G for d in range(1, G)]

    def siblings():
        return [(t + d) % T for d in range(1, T)]

    def copy(src, dst, ssem, rsem, dev):
        return pltpu.make_async_remote_copy(
            src_ref=src, dst_ref=dst, send_sem=ssem, recv_sem=rsem, device_id=dev, device_id_type=MESH
        )

    def arrived(ref, sem):
        pltpu.make_async_copy(ref, ref, sem).wait()

    def slot(s, ff, tt):
        if s == 0:
            return WA.at[tt, pl.ds(pl.multiple_of(ff * ka, ka), ka)]
        if s == 1:
            return WO.at[ff, pl.ds(pl.multiple_of(tt * ko, ko), ko)]
        if s == 2:
            return WU.at[tt, pl.ds(pl.multiple_of(ff * ku, ku), ku)]
        return WD.at[ff, pl.ds(pl.multiple_of(tt * kd, kd), kd)]

    def to_siblings(s, ff, src):
        for tt in siblings():
            copy(src, slot(s, ff, t), sd.at[s, ff], rd.at[s, ff], (r, f, tt)).start()

    def both_ways(s, ff, src):
        @pl.when(has_lo)
        def _():
            copy(src, slot(s, ff, t), sz.at[s, ff, 0], rz.at[s, ff], (r, f - 2, t)).start()

        @pl.when(has_hi)
        def _():
            copy(src, slot(s, ff, t), sz.at[s, ff, 1], rz.at[s, ff], (r, f + 2, t)).start()

    def kick(s):
        own = srcs[s]
        copy(own.at[1 - y], slot(s, f, t), sy.at[s], rz.at[s, f], (r, fy, t)).start()
        pltpu.make_async_copy(own.at[y], slot(s, f, t), loc.at[s]).start()
        both_ways(s, f, own.at[y])
        to_siblings(s, f, own.at[y])

    def kick2(s):
        arrived(slot(s, fy, t), rz.at[s, fy])
        both_ways(s, fy, slot(s, fy, t))
        to_siblings(s, fy, slot(s, fy, t))

    def place(j):
        k = (j + 1) // 2
        sg = 1 - 2 * (j % 2)
        return z + sg * k, z - sg

    def step(s, j):
        zs, nxt = place(j)

        @pl.when(jnp.logical_and(zs >= 0, zs < nz))
        def _():
            for yy in range(2):
                ff = 2 * zs + yy
                arrived(slot(s, ff, t), rz.at[s, ff])

                @pl.when(jnp.logical_and(nxt >= 0, nxt < nz))
                def _():
                    copy(
                        slot(s, ff, t), slot(s, ff, t), sz.at[s, ff, 0], rz.at[s, ff], (r, 2 * nxt + y, t)
                    ).start()

                to_siblings(s, ff, slot(s, ff, t))

    def steps(s, lo, hi):
        @pl.loop(lo, hi)
        def _(j):
            step(s, j)

    def from_siblings(s, ff):
        for tt in siblings():
            arrived(slot(s, ff, tt), rd.at[s, ff])

    def all_from_siblings(s):
        arrived(slot(s, f, t), loc.at[s])

        @pl.loop(0, 2 * nz)
        def _(ff):
            from_siblings(s, ff)

    last = 2 * nz - 1

    barrier = pltpu.get_barrier_semaphore()
    for m in others():
        pl.semaphore_signal(barrier, inc=1, device_id=member(m), device_id_type=MESH)
    for tt in siblings():
        pl.semaphore_signal(barrier, inc=1, device_id=(r, f, tt), device_id_type=MESH)

    @pl.when(has_lo)
    def _():
        pl.semaphore_signal(barrier, inc=1, device_id=(r, f - 2, t), device_id_type=MESH)

    @pl.when(has_hi)
    def _():
        pl.semaphore_signal(barrier, inc=1, device_id=(r, f + 2, t), device_id_type=MESH)

    pl.semaphore_wait(barrier, G + T - 2 + (z + nz - 1) // nz + (2 * nz - 2 - z) // nz)

    kick(0)
    kick(1)

    @pl.loop(0, win // TILE)
    def _(i):
        at = pl.ds(pl.multiple_of(i * TILE, TILE), TILE)
        x = tok[pl.ds(pl.multiple_of(start + i * TILE, TILE), TILE), :].astype(f32)
        x = x * lax.rsqrt(jnp.mean(x * x, axis=-1, keepdims=True) + norm_eps) * g1[...]
        nrm[g, at, :] = x.astype(bf16)

    kick2(0)
    for m in others():
        copy(nrm.at[g], nrm.at[g], sn.at[m], rn.at[g], member(m)).start()
    kick(2)
    kick2(1)
    steps(0, 1, last)
    kick(3)
    kick2(2)
    steps(1, 1, last)

    all_from_siblings(0)
    for m in others():
        arrived(nrm.at[m], rn.at[m])
    c = taps.shape[2]

    @pl.loop(0, G)
    def _(gs):
        x = nrm[gs]
        row = lax.broadcasted_iota(jnp.int32, (win, c), 0)
        for tt in range(T):
            prod = jnp.dot(x, WA[tt], preferred_element_type=f32) * asc[tt]
            gated = prod[:, c : 2 * c] * prod[:, :c]
            before = jnp.where(row == 0, 0.0, pltpu.roll(gated, 1, 0))
            after = jnp.where(row == win - 1, 0.0, pltpu.roll(gated, win - 1, 0))
            conv = taps[tt, 0:1] * before + taps[tt, 1:2] * gated + taps[tt, 2:3] * after
            hid[gs, :, tt * c : (tt + 1) * c] = (prod[:, 2 * c :] * conv).astype(bf16)

    all_from_siblings(1)

    @pl.loop(0, nz)
    def _(zs):
        @pl.loop(0, G)
        def _(gs):
            h = hid[gs, pl.ds(off, rows), :]
            for yy in range(2):
                p1[gs, zs, :, yy * cw : (yy + 1) * cw] = jnp.dot(
                    h, WO[2 * zs + yy], preferred_element_type=f32
                ).astype(bf16)

    kick2(3)
    for m in others():
        copy(p1.at[m], q1.at[g], s1.at[m], r1.at[g], member(m)).start()
    cut = (2 * last) // 3
    steps(2, 1, cut)

    for m in others():
        arrived(q1.at[m], r1.at[m])

    def total(p, q, zs, at):
        acc = p[g, zs, at, :].astype(f32)
        for m in others():
            acc = acc + q[m, zs, at, :].astype(f32)
        return acc

    @pl.loop(0, rows // TILE)
    def _(i):
        at = pl.ds(pl.multiple_of(i * TILE, TILE), TILE)
        here = pl.ds(pl.multiple_of(t * rows + i * TILE, TILE), TILE)
        ssq = jnp.zeros((TILE, 1), f32)
        for zs in range(nz):
            m = tok[here, zs * pw : (zs + 1) * pw].astype(f32) + total(p1, q1, zs, at) * oc[zs]
            mid32[zs, at, :] = m
            ssq = ssq + jnp.sum(m * m, axis=-1, keepdims=True)
        inv = lax.rsqrt(ssq / D + norm_eps)
        for zs in range(nz):
            cols = slice(zs * pw, (zs + 1) * pw)
            mid[g, at, cols] = (mid32[zs, at, :] * inv * g2[:, cols]).astype(bf16)

    steps(2, cut, cut + 1)
    for m in others():
        copy(mid.at[g], mid.at[g], sa.at[m], ra.at[g], member(m)).start()
    steps(2, cut + 1, last)
    cut2 = (last + 1) // 2
    steps(3, 1, cut2)

    all_from_siblings(2)
    for m in others():
        arrived(mid.at[m], ra.at[m])
    u = usc.shape[2]

    @pl.loop(0, G)
    def _(gs):
        x = mid[gs]
        for tt in range(T):
            upper = jnp.dot(x, WU[tt], preferred_element_type=f32) * usc[tt]
            act[gs, :, tt * u : (tt + 1) * u] = jnp.square(jnp.maximum(upper, 0.0)).astype(bf16)

    arrived(slot(3, f, t), loc.at[3])

    def down(j):
        zs, _ = place(j)

        @pl.when(jnp.logical_and(zs >= 0, zs < nz))
        def _():
            for yy in range(2):
                from_siblings(3, 2 * zs + yy)

            @pl.loop(0, G)
            def _(gs):
                x = act[gs]
                for yy in range(2):
                    p2[gs, zs, :, yy * cw : (yy + 1) * cw] = jnp.dot(
                        x, WD[2 * zs + yy], preferred_element_type=f32
                    ).astype(bf16)

            for m in others():
                copy(p2.at[m, zs], q2.at[g, zs], s2.at[m, zs], r2.at[g, zs], member(m)).start()

    @pl.loop(0, last)
    def _(j):
        @pl.when(j >= cut2)
        def _():
            step(3, j)

        down(j)

    @pl.loop(0, nz)
    def _(zs):
        for m in others():
            arrived(q2.at[m, zs], r2.at[m, zs])

    @pl.loop(0, rows // TILE)
    def _(i):
        at = pl.ds(pl.multiple_of(i * TILE, TILE), TILE)
        here = pl.ds(pl.multiple_of(t * rows + i * TILE, TILE), TILE)
        for zs in range(nz):
            out[here, zs * pw : (zs + 1) * pw] = (
                mid32[zs, at, :] + total(p2, q2, zs, at) * dc[zs]
            ).astype(bf16)

    def half(tt):
        return out.at[pl.ds(pl.multiple_of(tt * rows, rows), rows)]

    for tt in siblings():
        copy(half(t), half(t), so.at[tt], ro.at[t], (r, f, tt)).start()

    for s in range(4):
        own = srcs[s].at[y]
        arrived(own, sy.at[s])

        def gone(ff, k, s=s, own=own):
            arrived(own, sz.at[s, ff, k])

        for ff in (f, fy):
            pl.when(has_lo)(functools.partial(gone, ff, 0))
            pl.when(has_hi)(functools.partial(gone, ff, 1))

        @pl.loop(1, last)
        def _(j):
            zs, nxt = place(j)
            ok = jnp.logical_and(zs >= 0, zs < nz)

            @pl.when(jnp.logical_and(ok, jnp.logical_and(nxt >= 0, nxt < nz)))
            def _():
                for yy in range(2):
                    gone(2 * zs + yy, 0)

        @pl.loop(0, 2 * nz)
        def _(ff):
            for _ in siblings():
                arrived(own, sd.at[s, ff])

    for m in others():
        arrived(nrm.at[m], sn.at[m])
        arrived(p1.at[m], s1.at[m])
        arrived(mid.at[m], sa.at[m])

        @pl.loop(0, nz)
        def _(zs):
            arrived(p2.at[m, zs], s2.at[m, zs])

    for tt in siblings():
        arrived(half(tt), ro.at[tt])
        arrived(half(tt), so.at[tt])


def body(
    R, n_fs, T,
    tokens, mix_gain, value_weight, value_scale, inner_weight, inner_scale, outer_weight, outer_scale,
    conv_taps, out_weight, out_scale, mlp_gain, up_weight, up_scale, down_weight, down_scale,
):
    G, nz = 2 * R, n_fs // 2
    TOK, D = tokens.shape[1:]
    rows = TOK // T
    win = TOK if T == 1 else rows + HALO if T == 2 else rows + 2 * HALO
    r, f = lax.axis_index("rep"), lax.axis_index("fs")
    g = r * 2 + f % 2

    vs, us, os = value_scale.shape[0], up_scale.shape[0], out_scale.shape[0]
    tap = lax.dynamic_slice_in_dim(conv_taps, f * vs, vs, axis=1)
    packed = jnp.concatenate(
        [value_scale, inner_scale, outer_scale, tap[0], tap[1], tap[2], up_scale, out_scale, down_scale]
    )
    every = lax.all_gather(packed, ("tp", "fs"), axis=0, tiled=False).reshape(T, n_fs, -1)

    def block(v):
        return lax.dynamic_index_in_dim(v.reshape(T, G, -1), g, axis=1, keepdims=True)

    small = [block(every[:, :, i * vs : (i + 1) * vs]) for i in range(6)]
    asc = jnp.concatenate(small[:3], axis=2)
    taps = jnp.concatenate(small[3:], axis=1)
    usc = block(every[:, :, 6 * vs : 6 * vs + us])
    oc = every[0, :, 6 * vs + us : 6 * vs + us + os].reshape(nz, 1, -1)
    dc = every[0, :, 6 * vs + us + os :].reshape(nz, 1, -1)

    def col_blocks(w):
        w = lax.dynamic_index_in_dim(w.reshape(w.shape[0], R, -1), r, axis=1, keepdims=False)
        return w.reshape(w.shape[0], 2, -1).swapaxes(0, 1).astype(bf16)

    def row_blocks(w):
        w = lax.dynamic_index_in_dim(w.reshape(R, -1, w.shape[1]), r, axis=0, keepdims=False)
        return w.reshape(2, -1, w.shape[1]).astype(bf16)

    wa = jnp.concatenate([col_blocks(value_weight), col_blocks(inner_weight), col_blocks(outer_weight)], axis=2)
    wo, wu, wd = row_blocks(out_weight), col_blocks(up_weight), row_blocks(down_weight)
    ko, kd = wo.shape[1], wd.shape[1]
    pw = D // nz
    dma = pltpu.SemaphoreType.DMA
    vmem = pl.BlockSpec(memory_space=pltpu.VMEM)
    hbm = pl.BlockSpec(memory_space=pl.ANY)
    result = pl.pallas_call(
        functools.partial(kernel, nz, G, T, win, rows),
        out_shape=jax.ShapeDtypeStruct((TOK, D), bf16),
        in_specs=[vmem] * 8 + [hbm] * 4,
        out_specs=vmem,
        scratch_shapes=[
            pltpu.VMEM((T, D, wa.shape[2]), bf16),
            pltpu.VMEM((n_fs, T * ko, wo.shape[2]), bf16),
            pltpu.VMEM((T, D, wu.shape[2]), bf16),
            pltpu.VMEM((n_fs, T * kd, wd.shape[2]), bf16),
            pltpu.VMEM((G, win, D), bf16),
            pltpu.VMEM((G, win, T * ko), bf16),
            pltpu.VMEM((G, nz, rows, pw), bf16),
            pltpu.VMEM((G, nz, rows, pw), bf16),
            pltpu.VMEM((nz, rows, pw), f32),
            pltpu.VMEM((G, rows, D), bf16),
            pltpu.VMEM((G, rows, T * kd), bf16),
            pltpu.VMEM((G, nz, rows, pw), bf16),
            pltpu.VMEM((G, nz, rows, pw), bf16),
            dma((4, n_fs)),
            dma((4, n_fs)),
            dma((4, n_fs, 2)),
            dma((4, n_fs)),
            dma((4,)),
            dma((4,)),
            dma((G,)),
            dma((G,)),
            dma((G,)),
            dma((G,)),
            dma((G,)),
            dma((G,)),
            dma((G, nz)),
            dma((G, nz)),
            dma((T,)),
            dma((T,)),
        ],
        compiler_params=pltpu.CompilerParams(
            collective_id=0, has_side_effects=True, vmem_limit_bytes=65000000
        ),
    )(tokens[0], mix_gain[None], mlp_gain[None], asc, taps, usc, oc, dc, wa, wo, wu, wd)
    return result[None]


def solution(mesh):
    placed = (
        P(("rep", "fs"), None, None),
        P(),
        P("fs", "tp"),
        P(("tp", "fs")),
        P("fs", "tp"),
        P(("tp", "fs")),
        P("fs", "tp"),
        P(("tp", "fs")),
        P(None, "tp"),
        P("tp", "fs"),
        P("fs"),
        P(),
        P("fs", "tp"),
        P(("tp", "fs")),
        P("tp", "fs"),
        P("fs"),
    )
    sizes = (mesh.shape["rep"], mesh.shape["fs"], mesh.shape["tp"])
    return jax.shard_map(
        functools.partial(body, *sizes),
        mesh=mesh,
        in_specs=placed,
        out_specs=P(("rep", "fs"), None, None),
        check_vma=False,
    )
```

```python
import functools

import jax
import jax.numpy as jnp
from jax import lax
from jax.experimental import pallas as pl
from jax.experimental.pallas import tpu as pltpu
from jax.sharding import PartitionSpec as P

MESH = pl.DeviceIdType.MESH
norm_eps = 1e-06
HALO = 16
TILE = 16
f32 = jnp.float32
bf16 = jnp.bfloat16


def kernel(
    nz, G, T, win, rows, inside,
    tok, g1, g2, vectors, weights,
    out,
    WA, WO, WU, WD, nrm, hid, p1, q1, mid32, mid, act, p2, q2,
    staged, leaving, gathered,
    rz, rd, sz, sd, sy, loc, rn, sn, r1, s1, ra, sa, r2, s2, ro, so,
):
    if inside:
        packed, table, asc, taps, usc, oc, dc = gathered
    else:
        asc, taps, usc, oc, dc = vectors
    D = tok.shape[1]
    pw = D // nz
    cw = pw // 2
    r, f, t = lax.axis_index("rep"), lax.axis_index("fs"), lax.axis_index("tp")
    z, y = f // 2, f % 2
    fy = z * 2 + 1 - y
    g = r * 2 + y
    ka, ko, ku, kd = (w.shape[0] for w in leaving)
    stages = range(5 if inside else 4)
    has_lo, has_hi = z > 0, z < nz - 1
    if T == 2:
        start, off = t * (rows - HALO), t * HALO
    else:
        start = jnp.clip(t * rows - HALO, 0, tok.shape[0] - win)
        off = t * rows - start
    start, off = pl.multiple_of(start, HALO), pl.multiple_of(off, HALO)

    def member(m):
        return (m // 2, z * 2 + m % 2, t)

    def others():
        return [(g + d) % G for d in range(1, G)]

    def siblings():
        return [(t + d) % T for d in range(1, T)]

    def copy(src, dst, ssem, rsem, dev):
        return pltpu.make_async_remote_copy(
            src_ref=src, dst_ref=dst, send_sem=ssem, recv_sem=rsem, device_id=dev, device_id_type=MESH
        )

    def arrived(ref, sem):
        pltpu.make_async_copy(ref, ref, sem).wait()

    def slot(s, ff, tt):
        if s == 0:
            return WA.at[tt, pl.ds(pl.multiple_of(ff * ka, ka), ka)]
        if s == 1:
            return WO.at[ff, pl.ds(pl.multiple_of(tt * ko, ko), ko)]
        if s == 2:
            return WU.at[tt, pl.ds(pl.multiple_of(ff * ku, ku), ku)]
        if s == 3:
            return WD.at[ff, pl.ds(pl.multiple_of(tt * kd, kd), kd)]
        return table.at[ff, tt]

    def to_siblings(s, ff, src):
        for tt in siblings():
            copy(src, slot(s, ff, t), sd.at[s, ff], rd.at[s, ff], (r, f, tt)).start()

    def both_ways(s, ff, src):
        @pl.when(has_lo)
        def _():
            copy(src, slot(s, ff, t), sz.at[s, ff, 0], rz.at[s, ff], (r, f - 2, t)).start()

        @pl.when(has_hi)
        def _():
            copy(src, slot(s, ff, t), sz.at[s, ff, 1], rz.at[s, ff], (r, f + 2, t)).start()

    def fetches():
        for i, w in enumerate(weights):
            src, dst = weights[i], staged[i]
            if w.shape[1] > dst.shape[1]:
                n = dst.shape[1]
                src = src.at[:, pl.ds(pl.multiple_of(r * n, n), n)]
            elif w.shape[0] > dst.shape[0]:
                n = dst.shape[0]
                src = src.at[pl.ds(pl.multiple_of(r * n, n), n)]
            yield pltpu.make_async_copy(src, dst, loc.at[i])

    def round_stage(s):
        parts = {0: (0, 1, 2), 1: (3,), 2: (4,), 3: (5,)}[s]
        high = leaving[s].shape[0]
        for i in parts:
            pltpu.make_async_copy(staged[i], staged[i], loc.at[i]).wait()
        for yy in range(2):

            @pl.when(y == yy)
            def _():
                @pl.loop(0, high // 32)
                def _(k):
                    at = pl.ds(pl.multiple_of(k * 32, 32), 32)
                    for n, i in enumerate(parts):
                        if s in (0, 2):
                            wide = staged[i].shape[1] // 2
                            mine = staged[i][at, yy * wide : (yy + 1) * wide]
                            theirs = staged[i][at, (1 - yy) * wide : (2 - yy) * wide]
                        else:
                            wide = staged[i].shape[1]
                            mine = staged[i][pl.ds(pl.multiple_of(yy * high + k * 32, 32), 32), :]
                            theirs = staged[i][pl.ds(pl.multiple_of((1 - yy) * high + k * 32, 32), 32), :]
                        cols = slice(n * wide, (n + 1) * wide)
                        leaving[s][at, cols] = theirs.astype(bf16)
                        if s == 0:
                            WA[t, pl.ds(pl.multiple_of(f * ka + k * 32, 32), 32), cols] = mine.astype(bf16)
                        elif s == 1:
                            WO[f, pl.ds(pl.multiple_of(t * ko + k * 32, 32), 32), :] = mine.astype(bf16)
                        elif s == 2:
                            WU[t, pl.ds(pl.multiple_of(f * ku + k * 32, 32), 32), :] = mine.astype(bf16)
                        else:
                            WD[f, pl.ds(pl.multiple_of(t * kd + k * 32, 32), 32), :] = mine.astype(bf16)

    def kick(s):
        own = slot(s, f, t)
        copy(leaving[s] if s < 4 else own, own, sy.at[s], rz.at[s, f], (r, fy, t)).start()
        both_ways(s, f, own)
        to_siblings(s, f, own)

    def kick2(s):
        arrived(slot(s, fy, t), rz.at[s, fy])
        both_ways(s, fy, slot(s, fy, t))
        to_siblings(s, fy, slot(s, fy, t))

    def place(j):
        k = (j + 1) // 2
        sg = 1 - 2 * (j % 2)
        return z + sg * k, z - sg

    def step(s, j):
        zs, nxt = place(j)

        @pl.when(jnp.logical_and(zs >= 0, zs < nz))
        def _():
            for yy in range(2):
                ff = 2 * zs + yy
                arrived(slot(s, ff, t), rz.at[s, ff])

                @pl.when(jnp.logical_and(nxt >= 0, nxt < nz))
                def _():
                    copy(
                        slot(s, ff, t), slot(s, ff, t), sz.at[s, ff, 0], rz.at[s, ff], (r, 2 * nxt + y, t)
                    ).start()

                to_siblings(s, ff, slot(s, ff, t))

    def steps(s, lo, hi):
        @pl.loop(lo, hi)
        def _(j):
            step(s, j)

    def from_siblings(s, ff):
        for tt in siblings():
            arrived(slot(s, ff, tt), rd.at[s, ff])

    def all_from_siblings(s):
        @pl.loop(0, 2 * nz)
        def _(ff):
            from_siblings(s, ff)

    last = 2 * nz - 1

    for fetch in fetches():
        fetch.start()
    if inside:
        at_col = 0
        for v in vectors[:3]:
            packed[:, at_col : at_col + v.shape[1]] = v[...]
            at_col += v.shape[1]
        few = vectors[0].shape[1]
        for k in range(3):
            packed[:, at_col : at_col + few] = vectors[6][k : k + 1, pl.ds(pl.multiple_of(f * few, few), few)]
            at_col += few
        for v in vectors[3:6]:
            packed[:, at_col : at_col + v.shape[1]] = v[...]
            at_col += v.shape[1]
        table[f, t] = packed[...]

    barrier = pltpu.get_barrier_semaphore()
    for m in others():
        pl.semaphore_signal(barrier, inc=1, device_id=member(m), device_id_type=MESH)
    for tt in siblings():
        pl.semaphore_signal(barrier, inc=1, device_id=(r, f, tt), device_id_type=MESH)

    @pl.when(has_lo)
    def _():
        pl.semaphore_signal(barrier, inc=1, device_id=(r, f - 2, t), device_id_type=MESH)

    @pl.when(has_hi)
    def _():
        pl.semaphore_signal(barrier, inc=1, device_id=(r, f + 2, t), device_id_type=MESH)

    pl.semaphore_wait(barrier, G + T - 2 + (z + nz - 1) // nz + (2 * nz - 2 - z) // nz)

    round_stage(0)
    round_stage(1)
    kick(0)
    if inside:
        kick(4)
    kick(1)
    round_stage(2)
    round_stage(3)

    @pl.loop(0, win // TILE)
    def _(i):
        at = pl.ds(pl.multiple_of(i * TILE, TILE), TILE)
        x = tok[pl.ds(pl.multiple_of(start + i * TILE, TILE), TILE), :].astype(f32)
        x = x * lax.rsqrt(jnp.mean(x * x, axis=-1, keepdims=True) + norm_eps) * g1[...]
        nrm[g, at, :] = x.astype(bf16)

    kick2(0)
    if inside:
        kick2(4)
    for m in others():
        copy(nrm.at[g], nrm.at[g], sn.at[m], rn.at[g], member(m)).start()
    kick(2)
    kick2(1)
    steps(0, 1, last)
    if inside:
        steps(4, 1, last)
    kick(3)
    kick2(2)
    steps(1, 1, last)

    all_from_siblings(0)
    for m in others():
        arrived(nrm.at[m], rn.at[m])
    if inside:
        all_from_siblings(4)
        few, ups, outs = vectors[0].shape[1], vectors[3].shape[1], vectors[4].shape[1]
        wide = 3 * vectors[0].shape[1] * 2
        near = 2 * nz // G
        for tt in range(T):
            for j in range(near):
                row_of = table[g * near + j, tt]
                for k in range(3):
                    at_col = (k * near + j) * few
                    asc[tt, :, at_col : at_col + few] = row_of[:, k * few : (k + 1) * few]
                    taps[tt, k : k + 1, j * few : (j + 1) * few] = row_of[:, (3 + k) * few : (4 + k) * few]
                usc[tt, :, j * ups : (j + 1) * ups] = row_of[:, wide : wide + ups]
        for zs in range(nz):
            for yy in range(2):
                row_of = table[2 * zs + yy, 0]
                cols = slice(yy * outs, (yy + 1) * outs)
                oc[zs, :, cols] = row_of[:, wide + ups : wide + ups + outs]
                dc[zs, :, cols] = row_of[:, wide + ups + outs :]
    c = taps.shape[2]

    @pl.loop(0, G)
    def _(gs):
        x = nrm[gs]
        row = lax.broadcasted_iota(jnp.int32, (win, c), 0)
        for tt in range(T):
            prod = jnp.dot(x, WA[tt], preferred_element_type=f32) * asc[tt]
            gated = prod[:, c : 2 * c] * prod[:, :c]
            before = jnp.where(row == 0, 0.0, pltpu.roll(gated, 1, 0))
            after = jnp.where(row == win - 1, 0.0, pltpu.roll(gated, win - 1, 0))
            conv = taps[tt, 0:1] * before + taps[tt, 1:2] * gated + taps[tt, 2:3] * after
            hid[gs, :, tt * c : (tt + 1) * c] = (prod[:, 2 * c :] * conv).astype(bf16)

    all_from_siblings(1)

    @pl.loop(0, nz)
    def _(zs):
        @pl.loop(0, G)
        def _(gs):
            h = hid[gs, pl.ds(off, rows), :]
            for yy in range(2):
                p1[gs, zs, :, yy * cw : (yy + 1) * cw] = jnp.dot(
                    h, WO[2 * zs + yy], preferred_element_type=f32
                ).astype(bf16)

    kick2(3)
    for m in others():
        copy(p1.at[m], q1.at[g], s1.at[m], r1.at[g], member(m)).start()
    cut = (2 * last) // 3
    steps(2, 1, cut)

    for m in others():
        arrived(q1.at[m], r1.at[m])

    def total(p, q, zs, at):
        acc = p[g, zs, at, :].astype(f32)
        for m in others():
            acc = acc + q[m, zs, at, :].astype(f32)
        return acc

    @pl.loop(0, rows // TILE)
    def _(i):
        at = pl.ds(pl.multiple_of(i * TILE, TILE), TILE)
        here = pl.ds(pl.multiple_of(t * rows + i * TILE, TILE), TILE)
        ssq = jnp.zeros((TILE, 1), f32)
        for zs in range(nz):
            m = tok[here, zs * pw : (zs + 1) * pw].astype(f32) + total(p1, q1, zs, at) * oc[zs]
            mid32[zs, at, :] = m
            ssq = ssq + jnp.sum(m * m, axis=-1, keepdims=True)
        inv = lax.rsqrt(ssq / D + norm_eps)
        for zs in range(nz):
            cols = slice(zs * pw, (zs + 1) * pw)
            mid[g, at, cols] = (mid32[zs, at, :] * inv * g2[:, cols]).astype(bf16)

    steps(2, cut, cut + 1)
    for m in others():
        copy(mid.at[g], mid.at[g], sa.at[m], ra.at[g], member(m)).start()
    steps(2, cut + 1, last)
    cut2 = (last + 1) // 2
    steps(3, 1, cut2)

    all_from_siblings(2)
    for m in others():
        arrived(mid.at[m], ra.at[m])
    u = usc.shape[2]

    @pl.loop(0, G)
    def _(gs):
        x = mid[gs]
        for tt in range(T):
            upper = jnp.dot(x, WU[tt], preferred_element_type=f32) * usc[tt]
            act[gs, :, tt * u : (tt + 1) * u] = jnp.square(jnp.maximum(upper, 0.0)).astype(bf16)

    def down(j):
        zs, _ = place(j)

        @pl.when(jnp.logical_and(zs >= 0, zs < nz))
        def _():
            for yy in range(2):
                from_siblings(3, 2 * zs + yy)

            @pl.loop(0, G)
            def _(gs):
                x = act[gs]
                for yy in range(2):
                    p2[gs, zs, :, yy * cw : (yy + 1) * cw] = jnp.dot(
                        x, WD[2 * zs + yy], preferred_element_type=f32
                    ).astype(bf16)

            for m in others():
                copy(p2.at[m, zs], q2.at[g, zs], s2.at[m, zs], r2.at[g, zs], member(m)).start()

    @pl.loop(0, last)
    def _(j):
        @pl.when(j >= cut2)
        def _():
            step(3, j)

        down(j)

    @pl.loop(0, nz)
    def _(zs):
        for m in others():
            arrived(q2.at[m, zs], r2.at[m, zs])

    @pl.loop(0, rows // TILE)
    def _(i):
        at = pl.ds(pl.multiple_of(i * TILE, TILE), TILE)
        here = pl.ds(pl.multiple_of(t * rows + i * TILE, TILE), TILE)
        for zs in range(nz):
            out[here, zs * pw : (zs + 1) * pw] = (
                mid32[zs, at, :] + total(p2, q2, zs, at) * dc[zs]
            ).astype(bf16)

    def half(tt):
        return out.at[pl.ds(pl.multiple_of(tt * rows, rows), rows)]

    for tt in siblings():
        copy(half(t), half(t), so.at[tt], ro.at[t], (r, f, tt)).start()

    for s in stages:
        own = slot(s, f, t)
        arrived(own, sy.at[s])

        def gone(ff, k, s=s, own=own):
            arrived(own, sz.at[s, ff, k])

        for ff in (f, fy):
            pl.when(has_lo)(functools.partial(gone, ff, 0))
            pl.when(has_hi)(functools.partial(gone, ff, 1))

        @pl.loop(1, last)
        def _(j):
            zs, nxt = place(j)
            ok = jnp.logical_and(zs >= 0, zs < nz)

            @pl.when(jnp.logical_and(ok, jnp.logical_and(nxt >= 0, nxt < nz)))
            def _():
                for yy in range(2):
                    gone(2 * zs + yy, 0)

        @pl.loop(0, 2 * nz)
        def _(ff):
            for _ in siblings():
                arrived(own, sd.at[s, ff])

    for m in others():
        arrived(nrm.at[m], sn.at[m])
        arrived(p1.at[m], s1.at[m])
        arrived(mid.at[m], sa.at[m])

        @pl.loop(0, nz)
        def _(zs):
            arrived(p2.at[m, zs], s2.at[m, zs])

    for tt in siblings():
        arrived(half(tt), ro.at[tt])
        arrived(half(tt), so.at[tt])


def body(
    R, n_fs, T,
    tokens, mix_gain, value_weight, value_scale, inner_weight, inner_scale, outer_weight, outer_scale,
    conv_taps, out_weight, out_scale, mlp_gain, up_weight, up_scale, down_weight, down_scale,
):
    G, nz = 2 * R, n_fs // 2
    TOK, D = tokens.shape[1:]
    rows = TOK // T
    win = TOK if T == 1 else rows + HALO if T == 2 else rows + 2 * HALO
    r, f = lax.axis_index("rep"), lax.axis_index("fs")
    g = r * 2 + f % 2

    vs, us, os = value_scale.shape[0], up_scale.shape[0], out_scale.shape[0]
    inside = all(n % 128 == 0 for n in (vs, us, os))
    c, u = conv_taps.shape[1] // G, up_weight.shape[1] // G
    if inside:
        scales = (value_scale, inner_scale, outer_scale, up_scale, out_scale, down_scale)
        vectors = tuple(v[None] for v in scales) + (conv_taps,)
    else:
        tap = lax.dynamic_slice_in_dim(conv_taps, f * vs, vs, axis=1)
        packed = jnp.concatenate(
            [value_scale, inner_scale, outer_scale, tap[0], tap[1], tap[2], up_scale, out_scale, down_scale]
        )
        every = lax.all_gather(packed, ("tp", "fs"), axis=0, tiled=False).reshape(T, n_fs, -1)

        def block(v):
            return lax.dynamic_index_in_dim(v.reshape(T, G, -1), g, axis=1, keepdims=True)

        small = [block(every[:, :, i * vs : (i + 1) * vs]) for i in range(6)]
        asc = jnp.concatenate(small[:3], axis=2)
        taps = jnp.concatenate(small[3:], axis=1)
        usc = block(every[:, :, 6 * vs : 6 * vs + us])
        oc = every[0, :, 6 * vs + us : 6 * vs + us + os].reshape(nz, 1, -1)
        dc = every[0, :, 6 * vs + us + os :].reshape(nz, 1, -1)
        vectors = (asc, taps, usc, oc, dc)
    weights = (value_weight, inner_weight, outer_weight, out_weight, up_weight, down_weight)
    ka, ko, kd = value_weight.shape[0], out_weight.shape[0] // G, down_weight.shape[0] // G
    cw = out_weight.shape[1]
    rounded = [(ka, 3 * c), (ko, cw), (ka, u), (kd, cw)]
    staged = [(ka, 2 * c)] * 3 + [(2 * ko, cw), (ka, 2 * u), (2 * kd, cw)]
    gathered = ()
    if inside:
        L = 6 * vs + us + 2 * os
        small = [(1, L), (n_fs, T, 1, L), (T, 1, 3 * c), (T, 3, c), (T, 1, u), (nz, 1, 2 * cw), (nz, 1, 2 * cw)]
        gathered = tuple(pltpu.VMEM(shape, f32) for shape in small)
    pw = D // nz
    dma = pltpu.SemaphoreType.DMA
    vmem = pl.BlockSpec(memory_space=pltpu.VMEM)
    hbm = pl.BlockSpec(memory_space=pl.ANY)
    result = pl.pallas_call(
        functools.partial(kernel, nz, G, T, win, rows, inside),
        out_shape=jax.ShapeDtypeStruct((TOK, D), bf16),
        in_specs=[vmem] * 3 + [(vmem,) * len(vectors), (hbm,) * 6],
        out_specs=vmem,
        scratch_shapes=[
            pltpu.VMEM((T, D, 3 * c), bf16),
            pltpu.VMEM((n_fs, T * ko, cw), bf16),
            pltpu.VMEM((T, D, u), bf16),
            pltpu.VMEM((n_fs, T * kd, cw), bf16),
            pltpu.VMEM((G, win, D), bf16),
            pltpu.VMEM((G, win, T * ko), bf16),
            pltpu.VMEM((G, nz, rows, pw), bf16),
            pltpu.VMEM((G, nz, rows, pw), bf16),
            pltpu.VMEM((nz, rows, pw), f32),
            pltpu.VMEM((G, rows, D), bf16),
            pltpu.VMEM((G, rows, T * kd), bf16),
            pltpu.VMEM((G, nz, rows, pw), bf16),
            pltpu.VMEM((G, nz, rows, pw), bf16),
            tuple(pltpu.VMEM(shape, f32) for shape in staged),
            tuple(pltpu.VMEM(shape, bf16) for shape in rounded),
            gathered,
            dma((5, n_fs)),
            dma((5, n_fs)),
            dma((5, n_fs, 2)),
            dma((5, n_fs)),
            dma((5,)),
            dma((6,)),
            dma((G,)),
            dma((G,)),
            dma((G,)),
            dma((G,)),
            dma((G,)),
            dma((G,)),
            dma((G, nz)),
            dma((G, nz)),
            dma((T,)),
            dma((T,)),
        ],
        compiler_params=pltpu.CompilerParams(
            collective_id=0, has_side_effects=True, vmem_limit_bytes=65000000
        ),
    )(tokens[0], mix_gain[None], mlp_gain[None], vectors, weights)
    return result[None]


def solution(mesh):
    placed = (
        P(("rep", "fs"), None, None),
        P(),
        P("fs", "tp"),
        P(("tp", "fs")),
        P("fs", "tp"),
        P(("tp", "fs")),
        P("fs", "tp"),
        P(("tp", "fs")),
        P(None, "tp"),
        P("tp", "fs"),
        P("fs"),
        P(),
        P("fs", "tp"),
        P(("tp", "fs")),
        P("tp", "fs"),
        P("fs"),
    )
    sizes = (mesh.shape["rep"], mesh.shape["fs"], mesh.shape["tp"])
    return jax.shard_map(
        functools.partial(body, *sizes),
        mesh=mesh,
        in_specs=placed,
        out_specs=P(("rep", "fs"), None, None),
        check_vma=False,
    )
```

```python
import functools

import jax
import jax.numpy as jnp
from jax import lax
from jax.experimental import pallas as pl
from jax.experimental.pallas import tpu as pltpu
from jax.sharding import PartitionSpec as P

MESH = pl.DeviceIdType.MESH
norm_eps = 1e-06
HALO = 16
TILE = 16
f32 = jnp.float32
bf16 = jnp.bfloat16


def kernel(
    nz, G, T, win, rows, inside,
    tok, g1, g2, vectors, weights,
    out,
    WA, WO, WU, WD, nrm, hid, p1, q1, mid32, mid, act, p2, q2,
    staged, leaving, gathered,
    rz, rd, sz, sd, sy, loc, rn, sn, r1, s1, ra, sa, r2, s2, ro, so,
):
    if inside:
        packed, table, asc, taps, usc, oc, dc = gathered
    else:
        asc, taps, usc, oc, dc = vectors
    D = tok.shape[1]
    pw = D // nz
    cw = pw // 2
    r, f, t = lax.axis_index("rep"), lax.axis_index("fs"), lax.axis_index("tp")
    z, y = f // 2, f % 2
    fy = z * 2 + 1 - y
    g = r * 2 + y
    ka, ko, ku, kd = (w.shape[0] for w in leaving)
    stages = range(5 if inside else 4)
    has_lo, has_hi = z > 0, z < nz - 1
    if T == 2:
        start, off = t * (rows - HALO), t * HALO
    else:
        start = jnp.clip(t * rows - HALO, 0, tok.shape[0] - win)
        off = t * rows - start
    start, off = pl.multiple_of(start, HALO), pl.multiple_of(off, HALO)

    def member(m):
        return (m // 2, z * 2 + m % 2, t)

    def others():
        return [(g + d) % G for d in range(1, G)]

    def siblings():
        return [(t + d) % T for d in range(1, T)]

    def copy(src, dst, ssem, rsem, dev):
        return pltpu.make_async_remote_copy(
            src_ref=src, dst_ref=dst, send_sem=ssem, recv_sem=rsem, device_id=dev, device_id_type=MESH
        )

    def arrived(ref, sem):
        pltpu.make_async_copy(ref, ref, sem).wait()

    def slot(s, ff, tt):
        if s == 0:
            return WA.at[tt, pl.ds(pl.multiple_of(ff * ka, ka), ka)]
        if s == 1:
            return WO.at[ff, pl.ds(pl.multiple_of(tt * ko, ko), ko)]
        if s == 2:
            return WU.at[tt, pl.ds(pl.multiple_of(ff * ku, ku), ku)]
        if s == 3:
            return WD.at[ff, pl.ds(pl.multiple_of(tt * kd, kd), kd)]
        return table.at[ff, tt]

    def to_siblings(s, ff, src):
        for tt in siblings():
            copy(src, slot(s, ff, t), sd.at[s, ff], rd.at[s, ff], (r, f, tt)).start()

    def both_ways(s, ff, src):
        @pl.when(has_lo)
        def _():
            copy(src, slot(s, ff, t), sz.at[s, ff, 0], rz.at[s, ff], (r, f - 2, t)).start()

        @pl.when(has_hi)
        def _():
            copy(src, slot(s, ff, t), sz.at[s, ff, 1], rz.at[s, ff], (r, f + 2, t)).start()

    def fetches():
        for i, w in enumerate(weights):
            src, dst = weights[i], staged[i]
            if w.shape[1] > dst.shape[1]:
                n = dst.shape[1]
                src = src.at[:, pl.ds(pl.multiple_of(r * n, n), n)]
            elif w.shape[0] > dst.shape[0]:
                n = dst.shape[0]
                src = src.at[pl.ds(pl.multiple_of(r * n, n), n)]
            yield pltpu.make_async_copy(src, dst, loc.at[i])

    def round_stage(s):
        parts = {0: (0, 1, 2), 1: (3,), 2: (4,), 3: (5,)}[s]
        high = leaving[s].shape[0]
        for i in parts:
            pltpu.make_async_copy(staged[i], staged[i], loc.at[i]).wait()
        for yy in range(2):

            @pl.when(y == yy)
            def _():
                @pl.loop(0, high // 32)
                def _(k):
                    at = pl.ds(pl.multiple_of(k * 32, 32), 32)
                    for n, i in enumerate(parts):
                        if s in (0, 2):
                            wide = staged[i].shape[1] // 2
                            mine = staged[i][at, yy * wide : (yy + 1) * wide]
                            theirs = staged[i][at, (1 - yy) * wide : (2 - yy) * wide]
                        else:
                            wide = staged[i].shape[1]
                            mine = staged[i][pl.ds(pl.multiple_of(yy * high + k * 32, 32), 32), :]
                            theirs = staged[i][pl.ds(pl.multiple_of((1 - yy) * high + k * 32, 32), 32), :]
                        cols = slice(n * wide, (n + 1) * wide)
                        leaving[s][at, cols] = theirs.astype(bf16)
                        if s == 0:
                            WA[t, pl.ds(pl.multiple_of(f * ka + k * 32, 32), 32), cols] = mine.astype(bf16)
                        elif s == 1:
                            WO[f, pl.ds(pl.multiple_of(t * ko + k * 32, 32), 32), :] = mine.astype(bf16)
                        elif s == 2:
                            WU[t, pl.ds(pl.multiple_of(f * ku + k * 32, 32), 32), :] = mine.astype(bf16)
                        else:
                            WD[f, pl.ds(pl.multiple_of(t * kd + k * 32, 32), 32), :] = mine.astype(bf16)

    def kick(s):
        own = slot(s, f, t)
        copy(leaving[s] if s < 4 else own, own, sy.at[s], rz.at[s, f], (r, fy, t)).start()
        to_siblings(s, f, own)

    def kick2(s):
        both_ways(s, f, slot(s, f, t))
        arrived(slot(s, fy, t), rz.at[s, fy])
        both_ways(s, fy, slot(s, fy, t))
        to_siblings(s, fy, slot(s, fy, t))

    def place(j):
        k = (j + 1) // 2
        sg = 1 - 2 * (j % 2)
        return z + sg * k, z - sg

    def step(s, j):
        zs, nxt = place(j)

        @pl.when(jnp.logical_and(zs >= 0, zs < nz))
        def _():
            for k in range(2):
                ff = 2 * zs + (y + k) % 2
                arrived(slot(s, ff, t), rz.at[s, ff])

                @pl.when(jnp.logical_and(nxt >= 0, nxt < nz))
                def _():
                    copy(
                        slot(s, ff, t), slot(s, ff, t), sz.at[s, ff, 0], rz.at[s, ff], (r, 2 * nxt + y, t)
                    ).start()

                to_siblings(s, ff, slot(s, ff, t))

    def steps(s, lo, hi):
        @pl.loop(lo, hi)
        def _(j):
            step(s, j)

    def from_siblings(s, ff):
        for tt in siblings():
            arrived(slot(s, ff, tt), rd.at[s, ff])

    def all_from_siblings(s):
        @pl.loop(0, 2 * nz)
        def _(ff):
            from_siblings(s, ff)

    last = 2 * nz - 1

    for fetch in fetches():
        fetch.start()
    if inside:
        at_col = 0
        for v in vectors[:3]:
            packed[:, at_col : at_col + v.shape[1]] = v[...]
            at_col += v.shape[1]
        few = vectors[0].shape[1]
        for k in range(3):
            packed[:, at_col : at_col + few] = vectors[6][k : k + 1, pl.ds(pl.multiple_of(f * few, few), few)]
            at_col += few
        for v in vectors[3:6]:
            packed[:, at_col : at_col + v.shape[1]] = v[...]
            at_col += v.shape[1]
        table[f, t] = packed[...]

    round_stage(0)

    barrier = pltpu.get_barrier_semaphore()
    for m in others():
        pl.semaphore_signal(barrier, inc=1, device_id=member(m), device_id_type=MESH)
    for tt in siblings():
        pl.semaphore_signal(barrier, inc=1, device_id=(r, f, tt), device_id_type=MESH)

    @pl.when(has_lo)
    def _():
        pl.semaphore_signal(barrier, inc=1, device_id=(r, f - 2, t), device_id_type=MESH)

    @pl.when(has_hi)
    def _():
        pl.semaphore_signal(barrier, inc=1, device_id=(r, f + 2, t), device_id_type=MESH)

    pl.semaphore_wait(barrier, G + T - 2 + (z + nz - 1) // nz + (2 * nz - 2 - z) // nz)

    kick(0)
    both_ways(0, f, slot(0, f, t))
    if inside:
        kick(4)
    round_stage(1)
    kick(1)

    @pl.loop(0, win // TILE)
    def _(i):
        at = pl.ds(pl.multiple_of(i * TILE, TILE), TILE)
        x = tok[pl.ds(pl.multiple_of(start + i * TILE, TILE), TILE), :].astype(f32)
        x = x * lax.rsqrt(jnp.mean(x * x, axis=-1, keepdims=True) + norm_eps) * g1[...]
        nrm[g, at, :] = x.astype(bf16)

    for m in others():
        copy(nrm.at[g], nrm.at[g], sn.at[m], rn.at[g], member(m)).start()
    arrived(slot(0, fy, t), rz.at[0, fy])
    both_ways(0, fy, slot(0, fy, t))
    to_siblings(0, fy, slot(0, fy, t))
    round_stage(2)
    kick(2)
    round_stage(3)
    early = min(3, last)
    steps(0, 1, early)
    if inside:
        kick2(4)
    kick2(1)
    kick(3)
    steps(0, early, last)
    if inside:
        steps(4, 1, last)
    steps(1, 1, early)
    kick2(2)
    steps(1, early, last)

    all_from_siblings(0)
    for m in others():
        arrived(nrm.at[m], rn.at[m])
    if inside:
        all_from_siblings(4)
        few, ups, outs = vectors[0].shape[1], vectors[3].shape[1], vectors[4].shape[1]
        wide = 3 * vectors[0].shape[1] * 2
        near = 2 * nz // G
        for tt in range(T):
            for j in range(near):
                row_of = table[g * near + j, tt]
                for k in range(3):
                    at_col = (k * near + j) * few
                    asc[tt, :, at_col : at_col + few] = row_of[:, k * few : (k + 1) * few]
                    taps[tt, k : k + 1, j * few : (j + 1) * few] = row_of[:, (3 + k) * few : (4 + k) * few]
                usc[tt, :, j * ups : (j + 1) * ups] = row_of[:, wide : wide + ups]
        for zs in range(nz):
            for yy in range(2):
                row_of = table[2 * zs + yy, 0]
                cols = slice(yy * outs, (yy + 1) * outs)
                oc[zs, :, cols] = row_of[:, wide + ups : wide + ups + outs]
                dc[zs, :, cols] = row_of[:, wide + ups + outs :]
    c = taps.shape[2]

    @pl.loop(0, G)
    def _(gs):
        x = nrm[gs]
        row = lax.broadcasted_iota(jnp.int32, (win, c), 0)
        for tt in range(T):
            prod = jnp.dot(x, WA[tt], preferred_element_type=f32) * asc[tt]
            gated = prod[:, c : 2 * c] * prod[:, :c]
            before = jnp.where(row == 0, 0.0, pltpu.roll(gated, 1, 0))
            after = jnp.where(row == win - 1, 0.0, pltpu.roll(gated, win - 1, 0))
            conv = taps[tt, 0:1] * before + taps[tt, 1:2] * gated + taps[tt, 2:3] * after
            hid[gs, :, tt * c : (tt + 1) * c] = (prod[:, 2 * c :] * conv).astype(bf16)

    all_from_siblings(1)

    @pl.loop(0, nz)
    def _(zs):
        @pl.loop(0, G)
        def _(gs):
            h = hid[gs, pl.ds(off, rows), :]
            for yy in range(2):
                p1[gs, zs, :, yy * cw : (yy + 1) * cw] = jnp.dot(
                    h, WO[2 * zs + yy], preferred_element_type=f32
                ).astype(bf16)

    for m in others():
        copy(p1.at[m], q1.at[g], s1.at[m], r1.at[g], member(m)).start()
    cut = max(last - 2, early)
    steps(2, 1, early)
    kick2(3)
    steps(2, early, cut)

    for m in others():
        arrived(q1.at[m], r1.at[m])

    def total(p, q, zs, at):
        acc = p[g, zs, at, :].astype(f32)
        for m in others():
            acc = acc + q[m, zs, at, :].astype(f32)
        return acc

    @pl.loop(0, rows // TILE)
    def _(i):
        at = pl.ds(pl.multiple_of(i * TILE, TILE), TILE)
        here = pl.ds(pl.multiple_of(t * rows + i * TILE, TILE), TILE)
        ssq = jnp.zeros((TILE, 1), f32)
        for zs in range(nz):
            m = tok[here, zs * pw : (zs + 1) * pw].astype(f32) + total(p1, q1, zs, at) * oc[zs]
            mid32[zs, at, :] = m
            ssq = ssq + jnp.sum(m * m, axis=-1, keepdims=True)
        inv = lax.rsqrt(ssq / D + norm_eps)
        for zs in range(nz):
            cols = slice(zs * pw, (zs + 1) * pw)
            mid[g, at, cols] = (mid32[zs, at, :] * inv * g2[:, cols]).astype(bf16)

    for m in others():
        copy(mid.at[g], mid.at[g], sa.at[m], ra.at[g], member(m)).start()
    steps(2, cut, last)
    cut2 = (last + 1) // 2
    steps(3, 1, cut2)

    all_from_siblings(2)
    for m in others():
        arrived(mid.at[m], ra.at[m])
    u = usc.shape[2]

    @pl.loop(0, G)
    def _(gs):
        x = mid[gs]
        for tt in range(T):
            upper = jnp.dot(x, WU[tt], preferred_element_type=f32) * usc[tt]
            act[gs, :, tt * u : (tt + 1) * u] = jnp.square(jnp.maximum(upper, 0.0)).astype(bf16)

    def down(j):
        zs, _ = place(j)

        @pl.when(jnp.logical_and(zs >= 0, zs < nz))
        def _():
            for yy in range(2):
                from_siblings(3, 2 * zs + yy)

            @pl.loop(0, G)
            def _(gs):
                x = act[gs]
                for yy in range(2):
                    p2[gs, zs, :, yy * cw : (yy + 1) * cw] = jnp.dot(
                        x, WD[2 * zs + yy], preferred_element_type=f32
                    ).astype(bf16)

            for m in others():
                copy(p2.at[m, zs], q2.at[g, zs], s2.at[m, zs], r2.at[g, zs], member(m)).start()

    @pl.loop(0, last)
    def _(j):
        @pl.when(j >= cut2)
        def _():
            step(3, j)

        down(j)

    @pl.loop(0, nz)
    def _(zs):
        for m in others():
            arrived(q2.at[m, zs], r2.at[m, zs])

    @pl.loop(0, rows // TILE)
    def _(i):
        at = pl.ds(pl.multiple_of(i * TILE, TILE), TILE)
        here = pl.ds(pl.multiple_of(t * rows + i * TILE, TILE), TILE)
        for zs in range(nz):
            out[here, zs * pw : (zs + 1) * pw] = (
                mid32[zs, at, :] + total(p2, q2, zs, at) * dc[zs]
            ).astype(bf16)

    def half(tt):
        return out.at[pl.ds(pl.multiple_of(tt * rows, rows), rows)]

    for tt in siblings():
        copy(half(t), half(t), so.at[tt], ro.at[t], (r, f, tt)).start()

    for s in stages:
        own = slot(s, f, t)
        arrived(own, sy.at[s])

        def gone(ff, k, s=s, own=own):
            arrived(own, sz.at[s, ff, k])

        for ff in (f, fy):
            pl.when(has_lo)(functools.partial(gone, ff, 0))
            pl.when(has_hi)(functools.partial(gone, ff, 1))

        @pl.loop(1, last)
        def _(j):
            zs, nxt = place(j)
            ok = jnp.logical_and(zs >= 0, zs < nz)

            @pl.when(jnp.logical_and(ok, jnp.logical_and(nxt >= 0, nxt < nz)))
            def _():
                for yy in range(2):
                    gone(2 * zs + yy, 0)

        @pl.loop(0, 2 * nz)
        def _(ff):
            for _ in siblings():
                arrived(own, sd.at[s, ff])

    for m in others():
        arrived(nrm.at[m], sn.at[m])
        arrived(p1.at[m], s1.at[m])
        arrived(mid.at[m], sa.at[m])

        @pl.loop(0, nz)
        def _(zs):
            arrived(p2.at[m, zs], s2.at[m, zs])

    for tt in siblings():
        arrived(half(tt), ro.at[tt])
        arrived(half(tt), so.at[tt])


def body(
    R, n_fs, T,
    tokens, mix_gain, value_weight, value_scale, inner_weight, inner_scale, outer_weight, outer_scale,
    conv_taps, out_weight, out_scale, mlp_gain, up_weight, up_scale, down_weight, down_scale,
):
    G, nz = 2 * R, n_fs // 2
    TOK, D = tokens.shape[1:]
    rows = TOK // T
    win = TOK if T == 1 else rows + HALO if T == 2 else rows + 2 * HALO
    r, f = lax.axis_index("rep"), lax.axis_index("fs")
    g = r * 2 + f % 2

    vs, us, os = value_scale.shape[0], up_scale.shape[0], out_scale.shape[0]
    inside = all(n % 128 == 0 for n in (vs, us, os))
    c, u = conv_taps.shape[1] // G, up_weight.shape[1] // G
    if inside:
        scales = (value_scale, inner_scale, outer_scale, up_scale, out_scale, down_scale)
        vectors = tuple(v[None] for v in scales) + (conv_taps,)
    else:
        tap = lax.dynamic_slice_in_dim(conv_taps, f * vs, vs, axis=1)
        packed = jnp.concatenate(
            [value_scale, inner_scale, outer_scale, tap[0], tap[1], tap[2], up_scale, out_scale, down_scale]
        )
        every = lax.all_gather(packed, ("tp", "fs"), axis=0, tiled=False).reshape(T, n_fs, -1)

        def block(v):
            return lax.dynamic_index_in_dim(v.reshape(T, G, -1), g, axis=1, keepdims=True)

        small = [block(every[:, :, i * vs : (i + 1) * vs]) for i in range(6)]
        asc = jnp.concatenate(small[:3], axis=2)
        taps = jnp.concatenate(small[3:], axis=1)
        usc = block(every[:, :, 6 * vs : 6 * vs + us])
        oc = every[0, :, 6 * vs + us : 6 * vs + us + os].reshape(nz, 1, -1)
        dc = every[0, :, 6 * vs + us + os :].reshape(nz, 1, -1)
        vectors = (asc, taps, usc, oc, dc)
    weights = (value_weight, inner_weight, outer_weight, out_weight, up_weight, down_weight)
    ka, ko, kd = value_weight.shape[0], out_weight.shape[0] // G, down_weight.shape[0] // G
    cw = out_weight.shape[1]
    rounded = [(ka, 3 * c), (ko, cw), (ka, u), (kd, cw)]
    staged = [(ka, 2 * c)] * 3 + [(2 * ko, cw), (ka, 2 * u), (2 * kd, cw)]
    gathered = ()
    if inside:
        L = 6 * vs + us + 2 * os
        small = [(1, L), (n_fs, T, 1, L), (T, 1, 3 * c), (T, 3, c), (T, 1, u), (nz, 1, 2 * cw), (nz, 1, 2 * cw)]
        gathered = tuple(pltpu.VMEM(shape, f32) for shape in small)
    pw = D // nz
    dma = pltpu.SemaphoreType.DMA
    vmem = pl.BlockSpec(memory_space=pltpu.VMEM)
    hbm = pl.BlockSpec(memory_space=pl.ANY)
    result = pl.pallas_call(
        functools.partial(kernel, nz, G, T, win, rows, inside),
        out_shape=jax.ShapeDtypeStruct((TOK, D), bf16),
        in_specs=[vmem] * 3 + [(vmem,) * len(vectors), (hbm,) * 6],
        out_specs=vmem,
        scratch_shapes=[
            pltpu.VMEM((T, D, 3 * c), bf16),
            pltpu.VMEM((n_fs, T * ko, cw), bf16),
            pltpu.VMEM((T, D, u), bf16),
            pltpu.VMEM((n_fs, T * kd, cw), bf16),
            pltpu.VMEM((G, win, D), bf16),
            pltpu.VMEM((G, win, T * ko), bf16),
            pltpu.VMEM((G, nz, rows, pw), bf16),
            pltpu.VMEM((G, nz, rows, pw), bf16),
            pltpu.VMEM((nz, rows, pw), f32),
            pltpu.VMEM((G, rows, D), bf16),
            pltpu.VMEM((G, rows, T * kd), bf16),
            pltpu.VMEM((G, nz, rows, pw), bf16),
            pltpu.VMEM((G, nz, rows, pw), bf16),
            tuple(pltpu.VMEM(shape, f32) for shape in staged),
            tuple(pltpu.VMEM(shape, bf16) for shape in rounded),
            gathered,
            dma((5, n_fs)),
            dma((5, n_fs)),
            dma((5, n_fs, 2)),
            dma((5, n_fs)),
            dma((5,)),
            dma((6,)),
            dma((G,)),
            dma((G,)),
            dma((G,)),
            dma((G,)),
            dma((G,)),
            dma((G,)),
            dma((G, nz)),
            dma((G, nz)),
            dma((T,)),
            dma((T,)),
        ],
        compiler_params=pltpu.CompilerParams(
            collective_id=0, has_side_effects=True, vmem_limit_bytes=65000000
        ),
    )(tokens[0], mix_gain[None], mlp_gain[None], vectors, weights)
    return result[None]


def solution(mesh):
    placed = (
        P(("rep", "fs"), None, None),
        P(),
        P("fs", "tp"),
        P(("tp", "fs")),
        P("fs", "tp"),
        P(("tp", "fs")),
        P("fs", "tp"),
        P(("tp", "fs")),
        P(None, "tp"),
        P("tp", "fs"),
        P("fs"),
        P(),
        P("fs", "tp"),
        P(("tp", "fs")),
        P("tp", "fs"),
        P("fs"),
    )
    sizes = (mesh.shape["rep"], mesh.shape["fs"], mesh.shape["tp"])
    return jax.shard_map(
        functools.partial(body, *sizes),
        mesh=mesh,
        in_specs=placed,
        out_specs=P(("rep", "fs"), None, None),
        check_vma=False,
    )
```
